256 devices in a mesh: sp: 32 (over z, x), tp: 8 (over y, core).
Axes of the slice: x: 4, y: 4, z: 8, core: 2. Of those that a mesh axis runs over, the one named last changes fastest.
Arguments:
- tokens: bfloat16 [16384, 2048], P(('sp', 'tp')), may hold values from -40 to 40
- query_weight: bfloat16 [2048, 1024], P(None, 'tp'), may hold values from -0.1875 to 0.1875
- key_weight: bfloat16 [2048, 256], replicated, may hold values from -0.1875 to 0.1875
- value_weight: bfloat16 [2048, 256], replicated, may hold values from -0.125 to 0.125
- out_weight: bfloat16 [1024, 2048], replicated, may hold values from -0.1875 to 0.1875
- head_gain: float32 [128], replicated, may hold values from 0.1 to 1.9
- lambdas: float32 [8], P('tp'), may hold values from 0.3 to 0.8
Outputs:
- mixed: bfloat16 [16384, 2048], P(('sp', 'tp'))
The draws below stay inside these ranges and needn't reach their ends.
All inputs are finite; a program needn't handle non-finite values.
Results may differ from the reference program's by a relative error of at most 0.018.
The reference program's roundings to bfloat16 on the way count: a program that leaves them out, or rounds other values in their place, can miss the bound.
Values may be sent and summed in bfloat16 or wider, within the bound.
No kernel may reach another device: no remote copies, remote signals or barrier semaphores. Data moves between devices by JAX's collectives and lax.ppermute only.
A program may use at most 64 MiB of HBM per device.

```python
import jax
import jax.numpy as jnp
from jax import lax

D = 2048
H = 8
KVH = 2
DH = 64
DV = 128
TOK_DEV = 512
TOKENS = 16384


def draw_tokens(key, part):
    first_key = jax.random.fold_in(key, 11)
    second_key = jax.random.fold_in(key, 12)
    block_count = TOKENS // TOK_DEV
    shift = 0.6 * jax.random.normal(second_key, (block_count, D), jnp.float32)
    shifted = jnp.repeat(shift, TOK_DEV, axis=0)
    base = jax.random.normal(first_key, (TOKENS, D), jnp.float32)
    result = base + shifted
    return jnp.clip(result, -40.0, 40.0).astype(jnp.bfloat16)


def steps_of(own_key, shape, pieces, least, largest):
    gain = 1.0
    for position, parts in pieces:
        heights = jax.random.uniform(jax.random.fold_in(jax.random.fold_in(own_key, 6), position), (parts,), jnp.float32, least / len(pieces), largest / len(pieces))
        gain = gain * jnp.repeat(jnp.exp(heights), shape[position] // parts).reshape((-1,) + (1,) * (len(shape) - 1 - position))
    return gain


def gaussian(key, dims, width, limit, pieces=(), kind=jnp.bfloat16):
    values = width * jax.random.normal(key, dims, jnp.float32)
    if pieces:
        values = values * steps_of(key, dims, pieces, -0.22, 0.18)
    return jnp.clip(values, -limit, limit).astype(kind)


def setup_inputs(seed: int = 0) -> dict:
    key_list = jax.random.split(jax.random.key(seed), 8)
    tokens = draw_tokens(jax.random.fold_in(key_list[7], 71), 0)
    query_weight = gaussian(key_list[1], (D, H * 2 * DH), (D // 2) ** -0.5, 0.1875, ((1, 8),))
    key_weight = gaussian(key_list[2], (D, KVH * 2 * DH), (D // 2) ** -0.5, 0.1875)
    value_weight = gaussian(key_list[3], (D, KVH * DV), D ** -0.5, 0.125)
    out_weight = gaussian(key_list[4], (H * DV, D), (H * DV) ** -0.5, 0.1875)
    head_gain = jnp.clip(1.0 + 0.18 * jax.random.normal(key_list[5], (DV,), jnp.float32), 0.1, 1.9)
    lambdas = jnp.clip(0.3 + 0.5 * jax.random.uniform(key_list[6], (H,), jnp.float32) ** steps_of(key_list[6], (H,), ((0, 8),), -0.2, 0.2), 0.3, 0.8)
    return dict(tokens=tokens, query_weight=query_weight, key_weight=key_weight, value_weight=value_weight, out_weight=out_weight, head_gain=head_gain, lambdas=lambdas)


epsilon = 1e-06
rope_base = 10000.0
query_block = 128

def rotate(tensor_in, places):
    head_dim = tensor_in.shape[-1]
    half_dim = head_dim // 2
    frequency = rope_base ** (-(jnp.arange(half_dim, dtype=jnp.float32) * 2.0) / head_dim)
    angles = places[:, None] * frequency[None, :]
    angles = angles.reshape((places.shape[0],) + (1,) * (tensor_in.ndim - 2) + (half_dim,))
    cosine = jnp.cos(angles)
    sine_part = jnp.sin(angles)
    first = tensor_in[..., :half_dim]
    second = tensor_in[..., half_dim:]
    return jnp.concatenate([first * cosine - second * sine_part, first * sine_part + second * cosine], axis=-1)

def reference(tokens, query_weight, key_weight, value_weight, out_weight, head_gain, lambdas):
    places = jnp.arange(TOKENS).astype(jnp.float32)
    raw_queries = jnp.dot(tokens, query_weight, preferred_element_type=jnp.float32).reshape(TOKENS, H, 2, DH)
    queries = rotate(raw_queries, places).astype(jnp.bfloat16)
    raw_keys = jnp.dot(tokens, key_weight, preferred_element_type=jnp.float32).reshape(TOKENS, KVH, 2, DH)
    keys = rotate(raw_keys, places).astype(jnp.bfloat16)
    values = jnp.dot(tokens, value_weight, preferred_element_type=jnp.float32).astype(jnp.bfloat16).reshape(TOKENS, KVH, DV)
    group_size = H // KVH
    key_float = keys.astype(jnp.float32)
    value_float = values.astype(jnp.float32)
    score_scale = DH ** (-0.5)
    lambda_grid = lambdas.reshape(KVH, group_size)

    def one_block(query_rows):
        grouped = query_rows.astype(jnp.float32).reshape(query_block, KVH, group_size, 2, DH)
        scores = jnp.einsum('qagcd,kacd->cqagk', grouped, key_float) * score_scale
        row_max = lax.optimization_barrier(jnp.max(scores, axis=-1, keepdims=True))
        weights = jnp.exp(scores - row_max)
        row_sum = lax.optimization_barrier(jnp.sum(weights, axis=-1))
        rounded = lax.optimization_barrier(weights.astype(jnp.bfloat16)).astype(jnp.float32)
        numerator = jnp.einsum('cqagk,kav->cqagv', rounded, value_float)
        attended = numerator[0] / row_sum[0][..., None] - lambda_grid[None, :, :, None] * numerator[1] / row_sum[1][..., None]
        attended = attended.reshape(query_block, H, DV)
        mean_square = lax.optimization_barrier(jnp.mean(attended * attended, axis=-1, keepdims=True))
        normed = (attended * lax.rsqrt(mean_square + epsilon) * head_gain).astype(jnp.bfloat16)
        return normed.reshape(query_block, H * DV)
    blocks = queries.reshape(TOKENS // query_block, query_block, H, 2, DH)
    combined = lax.map(one_block, blocks).reshape(TOKENS, H * DV)
    return jnp.dot(combined, out_weight, preferred_element_type=jnp.float32).astype(jnp.bfloat16)
```

```python
import math, functools
from jax.experimental import pallas as pl
from jax.experimental.pallas import tpu as pltpu
import jax
import jax.numpy as jnp
from jax import lax
from jax.sharding import PartitionSpec as P

H = 8
DH = 64
DV = 128


epsilon = 1e-06
rope_base = 10000.0
fold_span = 2048


def joined_along(parts, dim):
    parts = jnp.moveaxis(parts, 0, dim)
    shape = parts.shape
    return parts.reshape(*shape[:dim], shape[dim] * shape[dim + 1], *shape[dim + 2 :])


def copy_for_each(x, axis):
    count = lax.axis_size(axis)
    return lax.all_to_all(jnp.broadcast_to(x[None], (count, *x.shape)), axis, 0, 0, tiled=True)


def gather_directly(x, axis, dim):
    return joined_along(copy_for_each(x, axis), dim)


def sent_together(arrays, axis, dim, along):
    ends, at = ([], 0)
    for a in arrays[:-1]:
        at += a.shape[along]
        ends.append(at)
    both = jnp.concatenate(arrays, axis=along)
    return tuple(jnp.split(lax.all_gather(both, axis, axis=dim, tiled=True), ends, axis=along))


def rotate(tensor_in, places):
    head_dim = tensor_in.shape[-1]
    half_dim = head_dim // 2
    frequency = rope_base ** (-(jnp.arange(half_dim, dtype=jnp.float32) * 2.0) / head_dim)
    angles = places[:, None] * frequency[None, :]
    angles = angles.reshape((places.shape[0],) + (1,) * (tensor_in.ndim - 2) + (half_dim,))
    cosine = jnp.cos(angles)
    sine_part = jnp.sin(angles)
    first = tensor_in[..., :half_dim]
    second = tensor_in[..., half_dim:]
    return jnp.concatenate(
        [first * cosine - second * sine_part, first * sine_part + second * cosine], axis=-1
    )


EXP_SCALE = math.log2(math.e) * 64 ** -0.5
ACC_ROWS = 136

def fold_block(q_ref, kv_ref, m_ref, acc_ref, start, kb, cb):
    n = q_ref.shape[1]
    k = kv_ref[pl.ds(start, kb), 0:128]
    v = kv_ref[pl.ds(start, kb), 128:256]
    vt = jnp.concatenate([v.T, jnp.ones((ACC_ROWS - 128, kb), jnp.bfloat16)], axis=0)
    def score(j):
        return jnp.dot(k, q_ref[:, j * cb:(j + 1) * cb], preferred_element_type=jnp.float32)
    nxt = score(0)
    nt = n // cb
    for j in range(nt):
        s = nxt
        if j + 1 < nt:
            nxt = score(j + 1)
        cols = slice(j * cb, (j + 1) * cb)
        old = m_ref[0:1, cols]
        new = jnp.maximum(old, jnp.max(s, axis=0, keepdims=True))
        m_ref[0:1, cols] = new
        p = jnp.exp2(s * EXP_SCALE - new * EXP_SCALE).astype(jnp.bfloat16)
        alpha = jnp.exp2((old - new) * EXP_SCALE)
        acc_ref[:, cols] = acc_ref[:, cols] * alpha + jnp.dot(vt, p, preferred_element_type=jnp.float32)

def attn_kernel(*refs, nkv, first, kb, cb):
    q_ref = refs[0]
    kvs = refs[1:1 + nkv]
    m_ref, acc_ref = refs[-2:]
    if first:
        m_ref[...] = jnp.full(m_ref.shape, -3e38, jnp.float32)
        acc_ref[...] = jnp.zeros(acc_ref.shape, jnp.float32)
    else:
        m_ref[...] = refs[1 + nkv][...]
        acc_ref[...] = refs[2 + nkv][...]
    for kv_ref in kvs:
        steps = kv_ref.shape[0] // kb
        def body(i, _):
            fold_block(q_ref, kv_ref, m_ref, acc_ref, pl.multiple_of(i * kb, kb), kb, cb)
            return 0
        lax.fori_loop(0, steps, body, 0)

def attn(q, kvs, carry=None, kb=1024, cb=512):
    n = q.shape[1]
    nk = sum(a.shape[0] for a in kvs)
    vm = pl.BlockSpec(memory_space=pltpu.VMEM)
    ops = [q, *kvs] + ([] if carry is None else list(carry))
    al = {} if carry is None else {len(ops) - 2: 0, len(ops) - 1: 1}
    return pl.pallas_call(
        functools.partial(attn_kernel, nkv=len(kvs), first=carry is None, kb=kb, cb=cb),
        out_shape=(jax.ShapeDtypeStruct((8, n), jnp.float32), jax.ShapeDtypeStruct((ACC_ROWS, n), jnp.float32)),
        in_specs=[vm] * len(ops), out_specs=(vm, vm), input_output_aliases=al,
        cost_estimate=pl.CostEstimate(flops=2 * nk * n * 256, transcendentals=nk * n, bytes_accessed=nk * 512),
        compiler_params=pltpu.CompilerParams(vmem_limit_bytes=56 * 2**20),
    )(*ops)


def local(tokens, query_weight, key_weight, value_weight, out_weight, head_gain, lambdas):
    heads_dev = query_weight.shape[1] // (2 * DH)
    kv_heads = key_weight.shape[1] // (2 * DH)
    group_size = H // kv_heads
    kv_index = lax.axis_index("tp") * heads_dev // group_size
    key_cols = lax.dynamic_slice_in_dim(key_weight, kv_index * (2 * DH), 2 * DH, 1)
    value_cols = lax.dynamic_slice_in_dim(value_weight, kv_index * DV, DV, 1)
    stacked = jnp.concatenate([query_weight, key_cols, value_cols], axis=1)
    projected = jnp.dot(
        gather_directly(tokens, "tp", 0), stacked, preferred_element_type=jnp.float32
    )
    seq_rows = projected.shape[0]
    places = (lax.axis_index("sp") * seq_rows + jnp.arange(seq_rows, dtype=jnp.int32)).astype(
        jnp.float32
    )
    query_cols = heads_dev * 2 * DH
    queries = rotate(projected[:, :query_cols].reshape(seq_rows, heads_dev, 2, DH), places).astype(
        jnp.bfloat16
    )
    key_rows = rotate(
        projected[:, query_cols : query_cols + 2 * DH].reshape(seq_rows, 2, DH), places
    )
    key_rows = key_rows.astype(jnp.bfloat16).reshape(seq_rows, 2 * DH)
    value_rows = projected[:, query_cols + 2 * DH :].astype(jnp.bfloat16)
    blank = jnp.zeros((DH, seq_rows * heads_dev), jnp.bfloat16)
    first_map = queries[:, :, 0].reshape(seq_rows * heads_dev, DH).T
    second_map = queries[:, :, 1].reshape(seq_rows * heads_dev, DH).T
    columns = jnp.concatenate(
        [jnp.concatenate([first_map, blank], 0), jnp.concatenate([blank, second_map], 0)], 1
    )
    gathered = lax.all_gather(
        jnp.concatenate([key_rows, value_rows], 1), "sp", axis=0, tiled=True
    )
    _, folded = attn(columns, [gathered])
    folded = folded.reshape(ACC_ROWS, 2, seq_rows, heads_dev)
    each = jnp.moveaxis(folded[:DV], 0, -1) / folded[DV][..., None]
    attended = each[0] - lambdas[None, :, None] * each[1]
    mean_square = jnp.mean(attended * attended, axis=-1, keepdims=True)
    normed = (attended * lax.rsqrt(mean_square + epsilon) * head_gain).astype(jnp.bfloat16)
    normed = normed.reshape(seq_rows, heads_dev * DV)
    regrouped = lax.all_to_all(normed, "tp", split_axis=0, concat_axis=1, tiled=True)
    return jnp.dot(regrouped, out_weight, preferred_element_type=jnp.float32).astype(jnp.bfloat16)


def solution(mesh):
    return jax.shard_map(
        local,
        mesh=mesh,
        in_specs=(P(("sp", "tp"), None), P(None, "tp"), P(), P(), P(), P(), P("tp")),
        out_specs=P(("sp", "tp"), None),
        check_vma=False,
    )
```

```python
import math, functools
from jax.experimental import pallas as pl
from jax.experimental.pallas import tpu as pltpu
import jax
import jax.numpy as jnp
from jax import lax
from jax.sharding import PartitionSpec as P

H = 8
DH = 64
DV = 128


epsilon = 1e-06
rope_base = 10000.0


def rotate(tensor_in, places):
    head_dim = tensor_in.shape[-1]
    half_dim = head_dim // 2
    frequency = rope_base ** (-(jnp.arange(half_dim, dtype=jnp.float32) * 2.0) / head_dim)
    angles = places[:, None] * frequency[None, :]
    angles = angles.reshape((places.shape[0],) + (1,) * (tensor_in.ndim - 2) + (half_dim,))
    cosine = jnp.cos(angles)
    sine_part = jnp.sin(angles)
    first = tensor_in[..., :half_dim]
    second = tensor_in[..., half_dim:]
    return jnp.concatenate(
        [first * cosine - second * sine_part, first * sine_part + second * cosine], axis=-1
    )


EXP_SCALE = math.log2(math.e) * 64 ** -0.5
ACC_ROWS = 136

def fold_block(q_ref, kv_ref, m_ref, acc_ref, start, kb, cb):
    n = q_ref.shape[1]
    k = kv_ref[pl.ds(start, kb), 0:128]
    v = kv_ref[pl.ds(start, kb), 128:256]
    vt = jnp.concatenate([v.T, jnp.ones((ACC_ROWS - 128, kb), jnp.bfloat16)], axis=0)
    def score(j):
        return jnp.dot(k, q_ref[:, j * cb:(j + 1) * cb], preferred_element_type=jnp.float32)
    nxt = score(0)
    nt = n // cb
    for j in range(nt):
        s = nxt
        if j + 1 < nt:
            nxt = score(j + 1)
        cols = slice(j * cb, (j + 1) * cb)
        old = m_ref[0:1, cols]
        new = jnp.maximum(old, jnp.max(s, axis=0, keepdims=True))
        m_ref[0:1, cols] = new
        p = jnp.exp2(s * EXP_SCALE - new * EXP_SCALE).astype(jnp.bfloat16)
        alpha = jnp.exp2((old - new) * EXP_SCALE)
        acc_ref[:, cols] = acc_ref[:, cols] * alpha + jnp.dot(vt, p, preferred_element_type=jnp.float32)

def attn_kernel(*refs, nkv, first, kb, cb):
    q_ref = refs[0]
    kvs = refs[1:1 + nkv]
    m_ref, acc_ref = refs[-2:]
    if first:
        m_ref[...] = jnp.full(m_ref.shape, -3e38, jnp.float32)
        acc_ref[...] = jnp.zeros(acc_ref.shape, jnp.float32)
    else:
        m_ref[...] = refs[1 + nkv][...]
        acc_ref[...] = refs[2 + nkv][...]
    for kv_ref in kvs:
        span = min(kb, kv_ref.shape[0])
        steps = kv_ref.shape[0] // span
        def body(i, _):
            fold_block(q_ref, kv_ref, m_ref, acc_ref, pl.multiple_of(i * span, span), span, cb)
            return 0
        lax.fori_loop(0, steps, body, 0)

def attn(q, kvs, carry=None, kb=1024, cb=512):
    n = q.shape[1]
    nk = sum(a.shape[0] for a in kvs)
    vm = pl.BlockSpec(memory_space=pltpu.VMEM)
    ops = [q, *kvs] + ([] if carry is None else list(carry))
    al = {} if carry is None else {len(ops) - 2: 0, len(ops) - 1: 1}
    return pl.pallas_call(
        functools.partial(attn_kernel, nkv=len(kvs), first=carry is None, kb=kb, cb=cb),
        out_shape=(jax.ShapeDtypeStruct((8, n), jnp.float32), jax.ShapeDtypeStruct((ACC_ROWS, n), jnp.float32)),
        in_specs=[vm] * len(ops), out_specs=(vm, vm), input_output_aliases=al,
        cost_estimate=pl.CostEstimate(flops=2 * nk * n * 256, transcendentals=nk * n, bytes_accessed=nk * 512),
        compiler_params=pltpu.CompilerParams(vmem_limit_bytes=56 * 2**20),
    )(*ops)


def mesh_sizes():
    return lax.axis_size("sp"), lax.axis_size("tp")


X_LEN = 4


def shifted(x, dz=0, dx=0, core=0):
    sp, tp = mesh_sizes()
    pairs = []
    for s in range(sp):
        for t in range(tp):
            z = (s // X_LEN + dz) % (sp // X_LEN)
            to = z * X_LEN + (s % X_LEN + dx) % X_LEN
            pairs.append((s * tp + t, to * tp + (t ^ core)))
    return lax.ppermute(x, ("sp", "tp"), pairs)


def same_core_groups():
    tp = lax.axis_size("tp")
    return [list(range(core, tp, 2)) for core in range(2)]


def turn(x, places):
    rows = x.shape[0]
    return rotate(x.reshape(rows, -1, DH), places).astype(jnp.bfloat16).reshape(rows, -1)


def finish_kernel(mine_ref, other_ref, lam_ref, gain_ref, out_ref):
    half = mine_ref.shape[1] // 2

    def joined(at):
        cols = slice(at, at + half)
        m1, m2 = mine_ref[DV + 1 : DV + 2, cols], other_ref[DV + 1 : DV + 2, cols]
        top = jnp.maximum(m1, m2)
        w1 = jnp.exp2((m1 - top) * EXP_SCALE)
        w2 = jnp.exp2((m2 - top) * EXP_SCALE)
        total = mine_ref[DV : DV + 1, cols] * w1 + other_ref[DV : DV + 1, cols] * w2
        return (mine_ref[0:DV, cols] * w1 + other_ref[0:DV, cols] * w2) / total

    attended = joined(0) - lam_ref[0] * joined(half)
    mean_square = jnp.mean(attended * attended, axis=0, keepdims=True)
    normed = attended * lax.rsqrt(mean_square + epsilon)
    out_ref[...] = (normed.T * gain_ref[...]).astype(jnp.bfloat16)


def local(tokens, query_weight, key_weight, value_weight, out_weight, head_gain, lambdas):
    rows = tokens.shape[0]
    sp_at, tp_at = lax.axis_index("sp"), lax.axis_index("tp")
    tp = lax.axis_size("tp")
    chips = tp // 2
    core = tp_at % 2
    kv_heads = key_weight.shape[1] // (2 * DH)
    groups = same_core_groups()
    base = sp_at * (rows * tp)

    own_places = (base + tp_at * rows + jnp.arange(rows, dtype=jnp.int32)).astype(jnp.float32)
    both = jnp.concatenate([key_weight, value_weight], axis=1)
    projected = jnp.dot(tokens, both, preferred_element_type=jnp.float32)
    own_keys = turn(projected[:, : key_weight.shape[1]], own_places)
    own_values = projected[:, key_weight.shape[1] :].astype(jnp.bfloat16)
    by_group = jnp.stack(
        [
            jnp.concatenate(
                [own_keys[:, 2 * DH * g : 2 * DH * (g + 1)], own_values[:, DV * g : DV * (g + 1)]], 1
            )
            for g in range(kv_heads)
        ]
    )
    to_chips = jnp.repeat(by_group, chips // kv_heads, axis=0)
    block = lax.all_to_all(to_chips, "tp", 0, 0, axis_index_groups=groups, tiled=True)
    block = block.reshape(chips * rows, 2 * DH + DV)

    held, block = lax.optimization_barrier((tokens, block))
    spread = jnp.broadcast_to(held[None], (chips, *held.shape))
    line = lax.all_to_all(spread, "tp", 0, 0, axis_index_groups=groups, tiled=True)
    line = line.reshape(chips * rows, tokens.shape[1])
    heads = jnp.concatenate([query_weight, shifted(query_weight, core=1)], axis=1)
    turned = (jnp.arange(chips, dtype=jnp.int32)[:, None] * 2 + core) * rows
    line_places = (base + turned + jnp.arange(rows, dtype=jnp.int32)[None]).reshape(-1)
    raw = jnp.dot(line, heads, preferred_element_type=jnp.float32)
    own_q = turn(raw, line_places.astype(jnp.float32))
    other_q = shifted(own_q, core=1)
    other_q = jnp.concatenate([other_q[:, 2 * DH :], other_q[:, : 2 * DH]], axis=1)
    low = jnp.where(core == 0, own_q, other_q).reshape(chips, 1, rows, 4 * DH)
    high = jnp.where(core == 0, other_q, own_q).reshape(chips, 1, rows, 4 * DH)
    queries = jnp.concatenate([low, high], axis=1).reshape(tp * rows, 4 * DH).T
    blank = jnp.zeros((DH, tp * rows), jnp.bfloat16)
    columns = jnp.concatenate(
        [
            jnp.concatenate([queries[:DH], blank, queries[2 * DH : 3 * DH], blank], 1),
            jnp.concatenate([blank, queries[DH : 2 * DH], blank, queries[3 * DH :]], 1),
        ],
        0,
    )

    row = jnp.concatenate([block] + [shifted(block, dx=d) for d in (1, 3, 2)], axis=0)
    half = row.shape[0] // 2
    up, down = shifted(row, dz=1), shifted(row, dz=-1)
    carry = attn(columns, [row])
    z_len = lax.axis_size("sp") // X_LEN
    for step in range(2, z_len // 2 + 2):
        last = step == z_len // 2
        more = step <= z_len // 2
        up, carry = lax.optimization_barrier((up, carry))
        next_up = shifted(up[:half] if last else up, dz=1) if more else None
        carry = attn(columns, [up], carry)
        down, carry = lax.optimization_barrier((down, carry))
        next_down = shifted(down[half:] if last else down, dz=-1) if more else None
        carry = attn(columns, [down], carry)
        up, down = next_up, next_down
    top, acc = carry

    acc = jnp.concatenate([acc[: DV + 1], top[:1], acc[DV + 2 :]], axis=0)
    split = acc.shape[1] // 2
    received = shifted(acc[:, split:], core=1)
    vm = pl.BlockSpec(memory_space=pltpu.VMEM)
    normed = pl.pallas_call(
        finish_kernel,
        out_shape=jax.ShapeDtypeStruct((tp * rows, DV), jnp.bfloat16),
        in_specs=[vm, vm, pl.BlockSpec(memory_space=pltpu.SMEM), vm],
        out_specs=vm,
    )(acc[:, :split], received, lambdas, head_gain.reshape(1, DV))
    regrouped = lax.all_to_all(normed, "tp", split_axis=0, concat_axis=1, tiled=True)
    return jnp.dot(regrouped, out_weight, preferred_element_type=jnp.float32).astype(jnp.bfloat16)


def solution(mesh):
    return jax.shard_map(
        local,
        mesh=mesh,
        in_specs=(P(("sp", "tp"), None), P(None, "tp"), P(), P(), P(), P(), P("tp")),
        out_specs=P(("sp", "tp"), None),
        check_vma=False,
    )
```

```python
import math, functools
from jax.experimental import pallas as pl
from jax.experimental.pallas import tpu as pltpu
import jax
import jax.numpy as jnp
from jax import lax
from jax.sharding import PartitionSpec as P

DH = 64
DV = 128


epsilon = 1e-06
rope_base = 10000.0


def rotate(tensor_in, places):
    head_dim = tensor_in.shape[-1]
    half_dim = head_dim // 2
    frequency = rope_base ** (-(jnp.arange(half_dim, dtype=jnp.float32) * 2.0) / head_dim)
    angles = places[:, None] * frequency[None, :]
    angles = angles.reshape((places.shape[0],) + (1,) * (tensor_in.ndim - 2) + (half_dim,))
    cosine = jnp.cos(angles)
    sine_part = jnp.sin(angles)
    first = tensor_in[..., :half_dim]
    second = tensor_in[..., half_dim:]
    return jnp.concatenate(
        [first * cosine - second * sine_part, first * sine_part + second * cosine], axis=-1
    )


EXP_SCALE = math.log2(math.e) * 64 ** -0.5
SUM_ROW, MAX_ROW, ACC_ROWS = DV, DV + 1, DV + 8


def fold_span(q_ref, kv_ref, acc_refs, start, span, width):
    k = kv_ref[pl.ds(start, span), 0:DV]
    v = kv_ref[pl.ds(start, span), DV : 2 * DV]
    raised = jnp.concatenate([v.T, jnp.ones((ACC_ROWS - DV, span), jnp.bfloat16)], axis=0)
    per_acc = acc_refs[0].shape[1] // width
    tiles = len(acc_refs) * per_acc

    def score(j):
        q = q_ref[:, j * width : (j + 1) * width]
        return jnp.dot(k, q, preferred_element_type=jnp.float32)

    ahead = score(0)
    for j in range(tiles):
        s = ahead
        if j + 1 < tiles:
            ahead = score(j + 1)
        acc_ref = acc_refs[j // per_acc]
        cols = slice(j % per_acc * width, (j % per_acc + 1) * width)
        old = acc_ref[MAX_ROW : MAX_ROW + 1, cols]
        new = jnp.maximum(old, jnp.max(s, axis=0, keepdims=True))
        p = jnp.exp2(s * EXP_SCALE - new * EXP_SCALE).astype(jnp.bfloat16)
        shrink = jnp.exp2((old - new) * EXP_SCALE)
        added = jnp.dot(raised, p, preferred_element_type=jnp.float32)
        acc_ref[:, cols] = acc_ref[:, cols] * shrink + added
        acc_ref[MAX_ROW : MAX_ROW + 1, cols] = new


def attend_kernel(q_ref, kv_ref, *refs, span, width):
    acc_refs = refs[-2:]
    if len(refs) == 2:
        for acc_ref in acc_refs:
            acc_ref[...] = jnp.zeros(acc_ref.shape, jnp.float32)
            acc_ref[MAX_ROW : MAX_ROW + 1, :] = jnp.full((1, acc_ref.shape[1]), -3e38, jnp.float32)
    else:
        for acc_ref, old_ref in zip(acc_refs, refs):
            acc_ref[...] = old_ref[...]

    def body(i, _):
        fold_span(q_ref, kv_ref, acc_refs, pl.multiple_of(i * span, span), span, width)
        return 0

    lax.fori_loop(0, kv_ref.shape[0] // span, body, 0)


def attend(q, kv, carry=(), span=512, width=512, lim=16):
    half = q.shape[1] // 2
    vm = pl.BlockSpec(memory_space=pltpu.VMEM)
    work = kv.shape[0] * q.shape[1]
    return pl.pallas_call(
        functools.partial(attend_kernel, span=min(span, kv.shape[0]), width=width),
        out_shape=(jax.ShapeDtypeStruct((ACC_ROWS, half), jnp.float32),) * 2,
        in_specs=[vm] * (2 + len(carry)),
        out_specs=(vm, vm),
        input_output_aliases={2: 0, 3: 1} if carry else {},
        cost_estimate=pl.CostEstimate(flops=512 * work, transcendentals=work, bytes_accessed=4 * work // 1024),
        compiler_params=pltpu.CompilerParams(vmem_limit_bytes=lim * 2**20),
    )(q, kv, *carry)


def mesh_sizes():
    return lax.axis_size("sp"), lax.axis_size("tp")


X_LEN = 4


def shifted(x, dz=0, dx=0, core=0):
    sp, tp = mesh_sizes()
    pairs = []
    for s in range(sp):
        for t in range(tp):
            z = (s // X_LEN + dz) % (sp // X_LEN)
            to = z * X_LEN + (s % X_LEN + dx) % X_LEN
            pairs.append((s * tp + t, to * tp + (t ^ core)))
    return lax.ppermute(x, ("sp", "tp"), pairs)


def same_core_groups():
    tp = lax.axis_size("tp")
    return [list(range(core, tp, 2)) for core in range(2)]


def plane_groups():
    sp, tp = mesh_sizes()
    return [
        [(z * X_LEN + x) * tp + 2 * y + core for x in range(X_LEN) for y in range(tp // 2)]
        for z in range(sp // X_LEN)
        for core in range(2)
    ]


def turn(x, places):
    rows = x.shape[0]
    return rotate(x.reshape(rows, -1, DH), places).astype(jnp.bfloat16).reshape(rows, -1)


def finish_kernel(mine_ref, other_ref, lam_ref, gain_ref, out_ref):
    half = mine_ref.shape[1] // 2

    def joined(at):
        cols = slice(at, at + half)
        m1, m2 = mine_ref[MAX_ROW : MAX_ROW + 1, cols], other_ref[MAX_ROW : MAX_ROW + 1, cols]
        top = jnp.maximum(m1, m2)
        w1 = jnp.exp2((m1 - top) * EXP_SCALE)
        w2 = jnp.exp2((m2 - top) * EXP_SCALE)
        sums = slice(SUM_ROW, SUM_ROW + 1)
        total = mine_ref[sums, cols] * w1 + other_ref[sums, cols] * w2
        return (mine_ref[0:DV, cols] * w1 + other_ref[0:DV, cols] * w2) / total

    attended = joined(0) - lam_ref[0] * joined(half)
    mean_square = jnp.mean(attended * attended, axis=0, keepdims=True)
    normed = attended * lax.rsqrt(mean_square + epsilon)
    out_ref[...] = (normed.T * gain_ref[...]).astype(jnp.bfloat16)


def local(tokens, query_weight, key_weight, value_weight, out_weight, head_gain, lambdas):
    rows = tokens.shape[0]
    sp_at, tp_at = lax.axis_index("sp"), lax.axis_index("tp")
    tp = lax.axis_size("tp")
    chips = tp // 2
    core = tp_at % 2
    kv_heads = key_weight.shape[1] // (2 * DH)
    groups = same_core_groups()
    base = sp_at * (rows * tp)

    own_places = (base + tp_at * rows + jnp.arange(rows, dtype=jnp.int32)).astype(jnp.float32)
    both = jnp.concatenate([key_weight, value_weight], axis=1)
    projected = jnp.dot(tokens, both, preferred_element_type=jnp.float32)
    own_keys = turn(projected[:, : key_weight.shape[1]], own_places)
    own_values = projected[:, key_weight.shape[1] :].astype(jnp.bfloat16)
    by_group = jnp.stack(
        [
            jnp.concatenate(
                [own_keys[:, 2 * DH * g : 2 * DH * (g + 1)], own_values[:, DV * g : DV * (g + 1)]], 1
            )
            for g in range(kv_heads)
        ]
    )
    to_plane = jnp.tile(jnp.repeat(by_group, chips // kv_heads, axis=0), (X_LEN, 1, 1))
    row = lax.all_to_all(
        to_plane, ("sp", "tp"), 0, 0, axis_index_groups=plane_groups(), tiled=True
    ).reshape(-1, 2 * DH + DV)
    up = shifted(row, dz=1)
    down = shifted(row, dz=-1)

    spread = jnp.broadcast_to(tokens[None], (chips, *tokens.shape))
    near = row
    line = lax.all_to_all(spread, "tp", 0, 0, axis_index_groups=groups, tiled=True)
    line = line.reshape(chips * rows, tokens.shape[1])
    heads = jnp.concatenate([query_weight, shifted(query_weight, core=1)], axis=1)
    turned = (jnp.arange(chips, dtype=jnp.int32)[:, None] * 2 + core) * rows
    line_places = (base + turned + jnp.arange(rows, dtype=jnp.int32)[None]).reshape(-1)
    raw = jnp.dot(line, heads, preferred_element_type=jnp.float32)
    own_q = turn(raw, line_places.astype(jnp.float32))
    other_q = shifted(own_q, core=1)
    other_q = jnp.concatenate([other_q[:, 2 * DH :], other_q[:, : 2 * DH]], axis=1)
    low = jnp.where(core == 0, own_q, other_q).reshape(chips, 1, rows, 4 * DH)
    high = jnp.where(core == 0, other_q, own_q).reshape(chips, 1, rows, 4 * DH)
    queries = jnp.concatenate([low, high], axis=1).reshape(tp * rows, 4 * DH).T
    blank = jnp.zeros((DH, tp * rows), jnp.bfloat16)
    columns = jnp.concatenate(
        [
            jnp.concatenate([queries[:DH], blank, queries[2 * DH : 3 * DH], blank], 1),
            jnp.concatenate([blank, queries[DH : 2 * DH], blank, queries[3 * DH :]], 1),
        ],
        0,
    )

    half = row.shape[0] // 2
    carry = attend(columns, near)
    z_len = lax.axis_size("sp") // X_LEN
    for step in range(2, z_len // 2 + 2):
        last = step == z_len // 2
        more = step <= z_len // 2
        up, carry = lax.optimization_barrier((up, carry))
        next_up = shifted(up[:half] if last else up, dz=1) if more else None
        carry = attend(columns, up, carry)
        down, carry = lax.optimization_barrier((down, carry))
        next_down = shifted(down[half:] if last else down, dz=-1) if more else None
        carry = attend(columns, down, carry)
        up, down = next_up, next_down
    mine, other = carry
    received = shifted(other, core=1)
    vm = pl.BlockSpec(memory_space=pltpu.VMEM)
    normed = pl.pallas_call(
        finish_kernel,
        out_shape=jax.ShapeDtypeStruct((tp * rows, DV), jnp.bfloat16),
        in_specs=[vm, vm, pl.BlockSpec(memory_space=pltpu.SMEM), vm],
        out_specs=vm,
        compiler_params=pltpu.CompilerParams(vmem_limit_bytes=16 * 2**20),
    )(mine, received, lambdas, head_gain.reshape(1, DV))
    regrouped = lax.all_to_all(normed, "tp", split_axis=0, concat_axis=1, tiled=True)
    return jnp.dot(regrouped, out_weight, preferred_element_type=jnp.float32).astype(jnp.bfloat16)


def solution(mesh):
    return jax.shard_map(
        local,
        mesh=mesh,
        in_specs=(P(("sp", "tp"), None), P(None, "tp"), P(), P(), P(), P(), P("tp")),
        out_specs=P(("sp", "tp"), None),
        check_vma=False,
    )
```

```python
import math, functools
from jax.experimental import pallas as pl
from jax.experimental.pallas import tpu as pltpu
import jax
import jax.numpy as jnp
from jax import lax
from jax.sharding import PartitionSpec as P

DH = 64
DV = 128


epsilon = 1e-06
rope_base = 10000.0


def rotate(tensor_in, places):
    head_dim = tensor_in.shape[-1]
    half_dim = head_dim // 2
    frequency = rope_base ** (-(jnp.arange(half_dim, dtype=jnp.float32) * 2.0) / head_dim)
    angles = places[:, None] * frequency[None, :]
    angles = angles.reshape((places.shape[0],) + (1,) * (tensor_in.ndim - 2) + (half_dim,))
    cosine = jnp.cos(angles)
    sine_part = jnp.sin(angles)
    first = tensor_in[..., :half_dim]
    second = tensor_in[..., half_dim:]
    return jnp.concatenate(
        [first * cosine - second * sine_part, first * sine_part + second * cosine], axis=-1
    )


EXP_SCALE = math.log2(math.e) * 64 ** -0.5
SUM_ROW, MAX_ROW, ACC_ROWS = DV, DV + 1, DV + 8


def fold_span(q_ref, kv_ref, acc_refs, start, span, width):
    k = kv_ref[pl.ds(start, span), 0:DV]
    v = kv_ref[pl.ds(start, span), DV : 2 * DV]
    raised = jnp.concatenate([v.T, jnp.ones((ACC_ROWS - DV, span), jnp.bfloat16)], axis=0)
    per_acc = acc_refs[0].shape[1] // width
    tiles = len(acc_refs) * per_acc

    def score(j):
        q = q_ref[:, j * width : (j + 1) * width]
        return jnp.dot(k, q, preferred_element_type=jnp.float32)

    ahead = score(0)
    for j in range(tiles):
        s = ahead
        if j + 1 < tiles:
            ahead = score(j + 1)
        acc_ref = acc_refs[j // per_acc]
        cols = slice(j % per_acc * width, (j % per_acc + 1) * width)
        old = acc_ref[MAX_ROW : MAX_ROW + 1, cols]
        new = jnp.maximum(old, jnp.max(s, axis=0, keepdims=True))
        p = jnp.exp2(s * EXP_SCALE - new * EXP_SCALE).astype(jnp.bfloat16)
        shrink = jnp.exp2((old - new) * EXP_SCALE)
        added = jnp.dot(raised, p, preferred_element_type=jnp.float32)
        acc_ref[:, cols] = acc_ref[:, cols] * shrink + added
        acc_ref[MAX_ROW : MAX_ROW + 1, cols] = new


def attend_kernel(q_ref, kv_ref, *refs, span, width):
    acc_refs = refs[-2:]
    if len(refs) == 2:
        for acc_ref in acc_refs:
            acc_ref[...] = jnp.zeros(acc_ref.shape, jnp.float32)
            acc_ref[MAX_ROW : MAX_ROW + 1, :] = jnp.full((1, acc_ref.shape[1]), -3e38, jnp.float32)
    else:
        for acc_ref, old_ref in zip(acc_refs, refs):
            acc_ref[...] = old_ref[...]

    def body(i, _):
        fold_span(q_ref, kv_ref, acc_refs, pl.multiple_of(i * span, span), span, width)
        return 0

    lax.fori_loop(0, kv_ref.shape[0] // span, body, 0)


def attend(q, kv, carry=(), span=512, width=512, lim=16):
    half = q.shape[1] // 2
    vm = pl.BlockSpec(memory_space=pltpu.VMEM)
    work = kv.shape[0] * q.shape[1]
    return pl.pallas_call(
        functools.partial(attend_kernel, span=min(span, kv.shape[0]), width=width),
        out_shape=(jax.ShapeDtypeStruct((ACC_ROWS, half), jnp.float32),) * 2,
        in_specs=[vm] * (2 + len(carry)),
        out_specs=(vm, vm),
        input_output_aliases={2: 0, 3: 1} if carry else {},
        cost_estimate=pl.CostEstimate(flops=512 * work, transcendentals=work, bytes_accessed=4 * work // 1024),
        compiler_params=pltpu.CompilerParams(vmem_limit_bytes=lim * 2**20),
    )(q, kv, *carry)


def mesh_sizes():
    return lax.axis_size("sp"), lax.axis_size("tp")


X_LEN = 4


def shifted(x, dz=0, dy=0, core=0):
    sp, tp = mesh_sizes()
    pairs = []
    for s in range(sp):
        for t in range(tp):
            to = (s + dz * X_LEN) % sp
            pairs.append((s * tp + t, to * tp + (t + 2 * dy) % tp ^ core))
    return lax.ppermute(x, ("sp", "tp"), pairs)


def plane_groups():
    sp, tp = mesh_sizes()
    return [
        [(z * X_LEN + x) * tp + 2 * y + core for x in range(X_LEN) for y in range(tp // 2)]
        for z in range(sp // X_LEN)
        for core in range(2)
    ]


def turn(x, places):
    rows = x.shape[0]
    return rotate(x.reshape(rows, -1, DH), places).astype(jnp.bfloat16).reshape(rows, -1)


def finish_kernel(mine_ref, other_ref, lam_ref, gain_ref, out_ref):
    half = mine_ref.shape[1] // 2

    def joined(at):
        cols = slice(at, at + half)
        m1, m2 = mine_ref[MAX_ROW : MAX_ROW + 1, cols], other_ref[MAX_ROW : MAX_ROW + 1, cols]
        top = jnp.maximum(m1, m2)
        w1 = jnp.exp2((m1 - top) * EXP_SCALE)
        w2 = jnp.exp2((m2 - top) * EXP_SCALE)
        sums = slice(SUM_ROW, SUM_ROW + 1)
        total = mine_ref[sums, cols] * w1 + other_ref[sums, cols] * w2
        return (mine_ref[0:DV, cols] * w1 + other_ref[0:DV, cols] * w2) / total

    attended = joined(0) - lam_ref[0] * joined(half)
    mean_square = jnp.mean(attended * attended, axis=0, keepdims=True)
    normed = attended * lax.rsqrt(mean_square + epsilon)
    out_ref[...] = (normed.T * gain_ref[...]).astype(jnp.bfloat16)


def local(tokens, query_weight, key_weight, value_weight, out_weight, head_gain, lambdas):
    rows = tokens.shape[0]
    sp_at, tp_at = lax.axis_index("sp"), lax.axis_index("tp")
    tp = lax.axis_size("tp")
    chips = tp // 2
    core = tp_at % 2
    kv_heads = key_weight.shape[1] // (2 * DH)
    base = sp_at * (rows * tp)

    own_places = (base + tp_at * rows + jnp.arange(rows, dtype=jnp.int32)).astype(jnp.float32)
    both = jnp.concatenate([key_weight, value_weight], axis=1)
    projected = jnp.dot(tokens, both, preferred_element_type=jnp.float32)
    own_keys = turn(projected[:, : key_weight.shape[1]], own_places)
    own_values = projected[:, key_weight.shape[1] :].astype(jnp.bfloat16)
    by_group = jnp.stack(
        [
            jnp.concatenate(
                [own_keys[:, 2 * DH * g : 2 * DH * (g + 1)], own_values[:, DV * g : DV * (g + 1)]], 1
            )
            for g in range(kv_heads)
        ]
    )
    to_plane = jnp.tile(jnp.repeat(by_group, chips // kv_heads, axis=0), (X_LEN, 1, 1))
    row = lax.all_to_all(
        to_plane, ("sp", "tp"), 0, 0, axis_index_groups=plane_groups(), tiled=True
    ).reshape(-1, 2 * DH + DV)
    up = shifted(row, dz=1)
    down = shifted(row, dz=-1)

    near = row
    pieces = [tokens]
    for d in range(1, chips):
        pieces.append(shifted(tokens, dy=d))
    heads = jnp.concatenate([query_weight, shifted(query_weight, core=1)], axis=1)
    raw = jnp.concatenate(
        [jnp.dot(p, heads, preferred_element_type=jnp.float32) for p in pieces[::-1]], axis=0
    )
    at = tp_at // 2
    raw = lax.dynamic_slice_in_dim(
        jnp.concatenate([raw, raw[: (chips - 1) * rows]]), (chips - 1 - at) * rows, chips * rows, 0
    )
    turned = (jnp.arange(chips, dtype=jnp.int32)[:, None] * 2 + core) * rows
    line_places = (base + turned + jnp.arange(rows, dtype=jnp.int32)[None]).reshape(-1)
    own_q = turn(raw, line_places.astype(jnp.float32))
    other_q = shifted(own_q, core=1)
    other_q = jnp.concatenate([other_q[:, 2 * DH :], other_q[:, : 2 * DH]], axis=1)
    low = jnp.where(core == 0, own_q, other_q).reshape(chips, 1, rows, 4 * DH)
    high = jnp.where(core == 0, other_q, own_q).reshape(chips, 1, rows, 4 * DH)
    queries = jnp.concatenate([low, high], axis=1).reshape(tp * rows, 4 * DH).T
    blank = jnp.zeros((DH, tp * rows), jnp.bfloat16)
    columns = jnp.concatenate(
        [
            jnp.concatenate([queries[:DH], blank, queries[2 * DH : 3 * DH], blank], 1),
            jnp.concatenate([blank, queries[DH : 2 * DH], blank, queries[3 * DH :]], 1),
        ],
        0,
    )

    half = row.shape[0] // 2
    carry = attend(columns, near)
    z_len = lax.axis_size("sp") // X_LEN
    for step in range(2, z_len // 2 + 2):
        last = step == z_len // 2
        more = step <= z_len // 2
        if step > 2:
            up, carry = lax.optimization_barrier((up, carry))
        next_up = shifted(up[:half] if last else up, dz=1) if more else None
        carry = attend(columns, up, carry)
        if step > 2:
            down, carry = lax.optimization_barrier((down, carry))
        next_down = shifted(down[half:] if last else down, dz=-1) if more else None
        carry = attend(columns, down, carry)
        up, down = next_up, next_down
    mine, other = carry
    received = shifted(other, core=1)
    vm = pl.BlockSpec(memory_space=pltpu.VMEM)
    normed = pl.pallas_call(
        finish_kernel,
        out_shape=jax.ShapeDtypeStruct((tp * rows, DV), jnp.bfloat16),
        in_specs=[vm, vm, pl.BlockSpec(memory_space=pltpu.SMEM), vm],
        out_specs=vm,
        compiler_params=pltpu.CompilerParams(vmem_limit_bytes=16 * 2**20),
    )(mine, received, lambdas, head_gain.reshape(1, DV))
    regrouped = lax.all_to_all(normed, "tp", split_axis=0, concat_axis=1, tiled=True)
    return jnp.dot(regrouped, out_weight, preferred_element_type=jnp.float32).astype(jnp.bfloat16)


def solution(mesh):
    return jax.shard_map(
        local,
        mesh=mesh,
        in_specs=(P(("sp", "tp"), None), P(None, "tp"), P(), P(), P(), P(), P("tp")),
        out_specs=P(("sp", "tp"), None),
        check_vma=False,
    )
```
